32 devices in a mesh: grp: 2 (over y), ep: 8 (over z, x), tp: 2 (over core).
Axes of the slice: x: 2, y: 2, z: 4, core: 2. Of those that a mesh axis runs over, the one named last changes fastest.
Arguments:
- tokens: bfloat16 [4096, 2048], P(('grp', 'ep', 'tp')), parts along dimension 0, may hold values from -6 to 6
- norm_gain: float32 [2048], replicated, may hold values from 0.1 to 1.9
- expert_ids: int32 [4096, 2], P(('grp', 'ep', 'tp')), parts along dimension 0, may hold values from 0 to 3, all different within a row; in each aligned block of 128 rows (0 to 127, 128 to 255, ...) at most 80 rows name the same one
- route_weights: float32 [4096, 2], P(('grp', 'ep', 'tp')), parts along dimension 0, may hold values from 0.1 to 0.9
- w_gate: bfloat16 [2048, 14336], P(None, ('ep', 'tp')), may hold values from -0.125 to 0.125
- w_up: bfloat16 [2048, 14336], P(None, ('ep', 'tp')), may hold values from -0.125 to 0.125
- w_down: bfloat16 [14336, 2048], P(('ep', 'tp')), may hold values from -0.09375 to 0.09375
Outputs:
- mixed_out: bfloat16 [4096, 2048], P(('grp', 'ep', 'tp')), parts along dimension 0
The draws below stay inside these ranges and needn't reach their ends.
There are 2 independent parts, one for each index of `grp`. The reference program is written for one: setup_inputs(seed, part) draws one part's arguments, and reference() takes and returns one part's arrays. A program takes and returns all parts, laid end to end along the dimension named above; an argument that names none is the same for every part. Nothing has to cross between parts.
Inputs may be any that keep to these rules, and one draw needn't show every extreme that they name: `expert_ids`: each row names 2 different experts. Among the rows of one device no expert is named more than 80 times, and in every draw some expert is named exactly 80 times by one device's rows.
All inputs are finite; a program needn't handle non-finite values.
Results may differ from the reference program's by a relative error of at most 0.01.
Values may be sent and summed in bfloat16 or wider, within the bound.
A program may use at most 128 MiB of HBM per device.

```python
import math
import jax
import jax.numpy as jnp
import numpy as np
from jax import lax

D = 2048
FF = 3584
TOP_K = 2
TOK_DEV = 128
EXPERTS = 4
CAP = 80
TOKENS = 2048
N_TP = 2


def level_of(stream_key, extent, pieces, low, largest):
    loudness = 1.0
    for dim, blocks in pieces:
        heights = jax.random.uniform(jax.random.fold_in(jax.random.fold_in(stream_key, 6), dim), (blocks,), jnp.float32, low / len(pieces), largest / len(pieces))
        loudness = loudness * jnp.repeat(jnp.exp(heights), extent[dim] // blocks).reshape((-1,) + (1,) * (len(extent) - 1 - dim))
    return loudness


def routed_block(stream_key, own, number, rows, amount, top, reach, slope):
    order = jax.random.permutation(stream_key, amount)
    heavy_load, common = shares(amount, rows * top, reach, slope, True), shares(amount, rows * top, reach, slope, False)
    places = jnp.arange(amount)

    def named(tallies, turn):
        used = int((tallies > 0).sum())
        fixed = max(1, used // 4)
        passed = fixed + (places - fixed + turn * (used - fixed)) % max(1, amount - fixed)
        return jnp.zeros((amount,), jnp.int32).at[order[jnp.where(places < fixed, places, passed)]].set(jnp.asarray(tallies, jnp.int32))

    tallies = jnp.where(number % 4 == 0, named(heavy_load, number // 4), named(common, number - number // 4 - 1))
    mixed = jax.random.permutation(jax.random.fold_in(own, 3), amount)
    donor, taker = mixed[0:amount // 2 * 2:2], mixed[1:amount // 2 * 2:2]
    margin = jnp.minimum(tallies[donor] - 1, reach - tallies[taker]) // 2
    margin = jnp.where((donor == order[0]) | (taker == order[0]) | (tallies[taker] == 0), 0, jnp.maximum(margin, 0))
    passed = jax.random.randint(jax.random.fold_in(own, 4), (amount // 2,), 0, 1 << 20) % (margin + 1)
    tallies = tallies.at[donor].add(-passed).at[taker].add(passed)
    members = jnp.searchsorted(jnp.cumsum(tallies), jnp.arange(rows * top), side="right").astype(jnp.int32)
    table = members.reshape(top, rows).T
    table = table[jax.random.permutation(jax.random.fold_in(own, 1), rows)]
    turn = jax.random.randint(jax.random.fold_in(own, 2), (rows, 1), 0, top)
    return jnp.take_along_axis(table, (jnp.arange(top)[None, :] + turn) % top, axis=1)


def shares(count, total, reach, lean, full):
    portions = [(1 << 20) // math.isqrt(rank ** lean) + 1 for rank in range(1, count + 1)]
    largest = reach if full else min(reach, max(-(-total // count), total * portions[0] // sum(portions)))
    least = 1 if total - largest >= count - 1 else 0
    given, surplus = [largest] + [least] * (count - 1), total - largest - least * (count - 1)
    while surplus > 0:
        free = [i for i in range(1, count) if given[i] < largest] or [i for i in range(1, count) if given[i] < reach]
        whole, budget = sum([portions[i] for i in free]), surplus
        for i in free:
            addition = min(reach - given[i], max(1, budget * portions[i] // whole), surplus)
            given[i] = given[i] + addition
            surplus = surplus - addition
    return np.array(given)


def noise(rng, shape, scale, reach, shards=(), kind=jnp.bfloat16):
    drawn = jax.random.normal(rng, shape, jnp.float32) * scale
    if len(shards) > 0:
        drawn = level_of(rng, shape, shards, -0.22, 0.18) * drawn
    return jnp.clip(drawn, min=-reach, max=reach).astype(kind)


def setup_inputs(seed: int = 0, part: int = 0) -> dict:
    arg_keys = jax.random.split(jax.random.key(seed), 8)
    part_splits = jax.random.split(jax.random.fold_in(arg_keys[7], part), 8)
    tokens = noise(part_splits[0], (TOKENS, D), 1.0, 6.0, ((0, 16),))
    norm_gain = jnp.clip(1.0 + 0.18 * jax.random.normal(arg_keys[1], (D,), jnp.float32), 0.1, 1.9)
    expert_ids_keys = jax.random.split(jax.random.fold_in(part_splits[2], 1), TOKENS // TOK_DEV)
    expert_ids_turns = jax.random.permutation(jax.random.fold_in(part_splits[2], 3), TOKENS // TOK_DEV)
    expert_ids = jax.vmap(lambda own, number: routed_block(jax.random.fold_in(part_splits[2], 2), own, number, TOK_DEV, EXPERTS, TOP_K, CAP, 2))(expert_ids_keys, expert_ids_turns).reshape((TOKENS, TOP_K))
    route_weights = jnp.clip(0.1 + 0.79999997 * jax.random.uniform(part_splits[3], (TOKENS, TOP_K), jnp.float32) ** level_of(part_splits[3], (TOKENS, TOP_K), ((0, 16),), -0.2, 0.2), 0.1, 0.9)
    w_gate = noise(arg_keys[4], (D, EXPERTS * FF), D ** -0.5, 0.125, ((1, 16),))
    w_up = noise(arg_keys[5], (D, EXPERTS * FF), D ** -0.5, 0.125, ((1, 16),))
    w_down = noise(arg_keys[6], (EXPERTS * FF, D), FF ** -0.5, 0.09375, ((0, 16),))
    return dict(tokens=tokens, norm_gain=norm_gain, expert_ids=expert_ids, route_weights=route_weights, w_gate=w_gate, w_up=w_up, w_down=w_down)


def reference(tokens, norm_gain, expert_ids, route_weights, w_gate, w_up, w_down):
    values = tokens.astype(jnp.float32)
    scale_rows = lax.rsqrt(lax.optimization_barrier(jnp.mean(values * values, axis=1, keepdims=True)) + 1e-06)
    normed = (values * scale_rows * norm_gain).astype(jnp.bfloat16)
    token_total = tokens.shape[0]
    sources = token_total // TOK_DEV
    per_source = expert_ids.reshape(sources, TOK_DEV * TOP_K)
    onehot = (per_source[:, :, None] == jnp.arange(EXPERTS, dtype=jnp.int32)[None, None, :]).astype(jnp.int32)
    earlier = jnp.cumsum(onehot, axis=1) - onehot
    slot_base = lax.optimization_barrier(jnp.sum(earlier * onehot, axis=2)).reshape(-1).astype(jnp.int32)
    flat_ids = expert_ids.reshape(-1).astype(jnp.int32)
    token_index = (jnp.arange(flat_ids.shape[0], dtype=jnp.int32) // TOP_K).astype(jnp.int32)
    source_index = (token_index // TOK_DEV).astype(jnp.int32)
    slot_index = jnp.remainder(slot_base + source_index, CAP).astype(jnp.int32)
    position = ((flat_ids * sources + source_index) * CAP + slot_index).astype(jnp.int32)
    slot_table = jnp.full((EXPERTS * sources * CAP,), token_total, jnp.int32).at[position].set(token_index)
    slot_table = slot_table.reshape(EXPERTS, sources * CAP)
    padded = jnp.concatenate([normed, jnp.zeros((1, normed.shape[1]), jnp.bfloat16)], axis=0)
    piece_width = FF // (2 * N_TP)

    def one_expert(inputs):
        expert, rows_index = inputs
        in_rows = padded[rows_index]
        first_col = (expert * FF).astype(jnp.int32)
        gate_part = jnp.dot(in_rows, lax.dynamic_slice_in_dim(w_gate, first_col, FF, 1), preferred_element_type=jnp.float32)
        up_part = jnp.dot(in_rows, lax.dynamic_slice_in_dim(w_up, first_col, FF, 1), preferred_element_type=jnp.float32)
        hidden = (jax.nn.silu(gate_part) * up_part).astype(jnp.bfloat16)
        down_rows = lax.dynamic_slice_in_dim(w_down, first_col, FF, 0)
        expert_total = jnp.zeros((in_rows.shape[0], normed.shape[1]), jnp.float32)
        for half_index in range(2):
            half_sum = jnp.zeros((in_rows.shape[0], normed.shape[1]), jnp.float32)
            for core_index in range(N_TP):
                begin = (half_index * N_TP + core_index) * piece_width
                partial_value = jnp.dot(hidden[:, begin:begin + piece_width], down_rows[begin:begin + piece_width], preferred_element_type=jnp.float32)
                half_sum = half_sum + lax.optimization_barrier(partial_value.astype(jnp.bfloat16)).astype(jnp.float32)
            expert_total = expert_total + lax.optimization_barrier(half_sum.astype(jnp.bfloat16)).astype(jnp.float32)
        return lax.optimization_barrier(expert_total.astype(jnp.bfloat16)).astype(jnp.float32)
    results = lax.map(one_expert, (jnp.arange(EXPERTS, dtype=jnp.int32), slot_table))
    picked = results.reshape(-1, normed.shape[1])[position].reshape(token_total, TOP_K, normed.shape[1])
    return lax.optimization_barrier(jnp.sum(picked * route_weights[:, :, None], axis=1)).astype(jnp.bfloat16)
```

```python
import functools

import jax
import jax.numpy as jnp
from jax import lax
from jax.experimental import pallas as pl
from jax.experimental.pallas import tpu as pltpu
from jax.sharding import PartitionSpec as P

MESH = pl.DeviceIdType.MESH
LANE = 128


def mix_index(first, second, count):
    total = first * 0
    bit = 1
    while bit < count:
        one, two = (first // bit) % 2, (second // bit) % 2
        total = total + bit * (one + two - 2 * one * two)
        bit *= 2
    return total


def kernel(
    experts, cap,
    tok_ref, gain_ref, ids_ref, ids_t_ref, weight_ref, gate_ref, up_ref, down_ref,
    out_ref,
    norm, xs, xa, hid, po, rd, cx, rx, fo, ret, wgu, wd,
    gate_sem, up_sem, down_sem, own_sem,
    z_send, z_recv, x_send, x_recv, d_send, d_recv, e_send, e_recv,
    r_send, r_recv, v_send, v_recv, w_send, w_recv,
):
    ep, c = lax.axis_index("ep"), lax.axis_index("tp")
    p, h = ep // 2, ep % 2
    toks, width = tok_ref.shape
    tiles = wgu.shape[0]
    across = {"ep": 2 * p + 1 - h, "tp": c}
    beside = {"ep": ep, "tp": 1 - c}

    def plane(q):
        return {"ep": 2 * q + h, "tp": c}

    barrier = pltpu.get_barrier_semaphore()

    def greet(k, carry):
        pl.semaphore_signal(barrier, inc=1, device_id=plane(mix_index(p, k, experts)), device_id_type=MESH)
        return carry

    lax.fori_loop(1, experts, greet, 0)
    pl.semaphore_signal(barrier, inc=1, device_id=across, device_id_type=MESH)
    pl.semaphore_signal(barrier, inc=1, device_id=beside, device_id_type=MESH)

    def gate_copy(j):
        return pltpu.make_async_copy(
            gate_ref.at[:, pl.ds(j * LANE, LANE)], wgu.at[j, :, pl.ds(0, LANE)], gate_sem.at[j])

    def up_copy(j):
        return pltpu.make_async_copy(
            up_ref.at[:, pl.ds(j * LANE, LANE)], wgu.at[j, :, pl.ds(LANE, LANE)], up_sem.at[j])

    down_copy = pltpu.make_async_copy(down_ref, wd, down_sem)
    for j in range(tiles):
        gate_copy(j).start()
        up_copy(j).start()
    down_copy.start()

    values = tok_ref[...].astype(jnp.float32)
    scale_rows = lax.rsqrt(jnp.mean(values * values, axis=1, keepdims=True) + 1e-06)
    norm[...] = (values * scale_rows * gain_ref[...]).astype(jnp.bfloat16)

    row = lax.broadcasted_iota(jnp.int32, (toks, toks), 0)
    col = lax.broadcasted_iota(jnp.int32, (toks, toks), 1)
    before = (row < col).astype(jnp.float32).astype(jnp.bfloat16)
    slots = lax.broadcasted_iota(jnp.int32, (cap, toks), 0).astype(jnp.float32)

    def fill(e, carry):
        named = ((ids_t_ref[0:1, :] == e) | (ids_t_ref[1:2, :] == e)).astype(jnp.float32)
        rank = jnp.dot(
            jnp.broadcast_to(named, (16, toks)).astype(jnp.bfloat16), before,
            preferred_element_type=jnp.float32)[0:1, :]
        pick = jnp.where(slots == rank, named, 0.0).astype(jnp.bfloat16)
        xs[e] = jnp.dot(pick, norm[...], preferred_element_type=jnp.float32).astype(jnp.bfloat16)
        return carry

    lax.fori_loop(0, experts, fill, 0)
    pl.semaphore_wait(barrier, experts + 1)

    def remote(src, dst, send, recv, target):
        return pltpu.make_async_remote_copy(
            src_ref=src, dst_ref=dst, send_sem=send, recv_sem=recv, device_id=target, device_id_type=MESH)

    def z_copy(k):
        q = mix_index(p, k, experts)
        return remote(xs.at[q], xa.at[4 * p + 2 * h + c], z_send.at[k], z_recv.at[k], plane(q))

    def z_land(k):
        q = mix_index(p, k, experts)
        return remote(xs.at[q], xa.at[4 * q + 2 * h + c], z_send.at[k], z_recv.at[k], plane(q))

    own_copy = pltpu.make_async_copy(xs.at[p], xa.at[4 * p + 2 * h + c], own_sem)

    def mine(k, half, core):
        return xa.at[4 * mix_index(p, k, experts) + 2 * half + core]

    def x_copy(k):
        return remote(mine(k, h, c), mine(k, h, c), x_send.at[k], x_recv.at[k], across)

    def x_land(k):
        return remote(mine(k, h, c), mine(k, 1 - h, c), x_send.at[k], x_recv.at[k], across)

    def d_copy(k):
        return remote(mine(k, h, c), mine(k, h, c), d_send.at[k], d_recv.at[k], beside)

    def d_land(k):
        return remote(mine(k, h, c), mine(k, h, 1 - c), d_send.at[k], d_recv.at[k], beside)

    def e_copy(k):
        return remote(mine(k, 1 - h, c), mine(k, 1 - h, c), e_send.at[k], e_recv.at[k], beside)

    def e_land(k):
        return remote(mine(k, 1 - h, c), mine(k, 1 - h, 1 - c), e_send.at[k], e_recv.at[k], beside)

    def r_copy(k, half):
        return remote(
            po.at[4 * k + 2 * half + 1 - c], rd.at[2 * k + half],
            r_send.at[2 * k + half], r_recv.at[2 * k + half], beside)

    def v_copy(k):
        return remote(cx.at[2 * k + 1 - h], rx.at[k], v_send.at[k], v_recv.at[k], across)

    def w_copy(k):
        return remote(fo.at[k], ret.at[p], w_send.at[k], w_recv.at[k], plane(mix_index(p, k, experts)))

    def w_land(k):
        q = mix_index(p, k, experts)
        return remote(fo.at[k], ret.at[q], w_send.at[k], w_recv.at[k], plane(q))

    own_copy.start()

    def send(k, carry):
        z_copy(k).start()
        return carry

    lax.fori_loop(1, experts, send, 0)
    own_copy.wait()

    def compute(k):
        first = 4 * mix_index(p, k, experts)

        def gate_up(j, carry):
            rows = xa[pl.ds(first, 4)].reshape(4 * cap, width)
            both = jnp.dot(rows, wgu[j], preferred_element_type=jnp.float32)
            gate, up = both[:, :LANE], both[:, LANE:]
            hid[:, pl.ds(pl.multiple_of(j * LANE, LANE), LANE)] = (
                gate / (1.0 + jnp.exp(-gate)) * up).astype(jnp.bfloat16)
            return carry

        lax.fori_loop(0, tiles, gate_up, 0)
        step = 2 * LANE

        def down(n, carry):
            place = pl.ds(pl.multiple_of(n * step, step), step)
            part = jnp.dot(hid[...], wd[:, place], preferred_element_type=jnp.float32)
            po[pl.ds(4 * k, 4), :, place] = part.astype(jnp.bfloat16).reshape(4, cap, step)
            return carry

        lax.fori_loop(0, width // step, down, 0)

    def finish(k):
        v_copy(k).wait_recv()
        total = (cx[2 * k + h].astype(jnp.float32) + rx[k].astype(jnp.float32)).astype(jnp.bfloat16)

        @pl.when(k == 0)
        def _():
            ret[p] = total

        @pl.when(k > 0)
        def _():
            fo[k] = total
            w_copy(k).start()

    def stage(i, carry):
        @pl.when(i < experts)
        def _():
            @pl.when(i > 0)
            def _():
                z_land(i).wait_recv()

            x_copy(i).start()
            d_copy(i).start()

        @pl.when(i > 0)
        def _():
            k = i - 1
            x_land(k).wait_recv()
            e_copy(k).start()

            @pl.when(k == 0)
            def _():
                for j in range(tiles):
                    gate_copy(j).wait()
                    up_copy(j).wait()
                down_copy.wait()

            d_land(k).wait_recv()
            e_land(k).wait_recv()
            compute(k)
            for half in range(2):
                r_copy(k, half).start()

            @pl.when(k > 0)
            def _():
                finish(k - 1)

            for half in range(2):
                r_copy(k, half).wait_recv()
                cx[2 * k + half] = (
                    po[4 * k + 2 * half + c].astype(jnp.float32) + rd[2 * k + half].astype(jnp.float32)
                ).astype(jnp.bfloat16)
            v_copy(k).start()

        return carry

    lax.fori_loop(0, experts + 1, stage, 0)
    finish(experts - 1)

    def settle(k, carry):
        x_copy(k).wait_send()
        d_copy(k).wait_send()
        e_copy(k).wait_send()
        r_copy(k, 0).wait_send()
        r_copy(k, 1).wait_send()
        v_copy(k).wait_send()

        @pl.when(k > 0)
        def _():
            z_copy(k).wait_send()
            w_copy(k).wait_send()
            w_land(k).wait_recv()

        return carry

    after = (col < row).astype(jnp.float32).astype(jnp.bfloat16)

    def place_of(e, places):
        hits = [(ids_ref[:, n:n + 1] == e).astype(jnp.float32) for n in range(2)]
        rank = jnp.dot(
            after, jnp.broadcast_to(hits[0] + hits[1], (toks, LANE)).astype(jnp.bfloat16),
            preferred_element_type=jnp.float32)[:, 0:1]
        spot = rank + lax.convert_element_type(e * cap, jnp.float32)
        return tuple(old + hit * spot for old, hit in zip(places, hits))

    zero = jnp.zeros((toks, 1), jnp.float32)
    places = lax.fori_loop(0, experts, place_of, (zero, zero))
    lax.fori_loop(0, experts, settle, 0)
    lanes = lax.broadcasted_iota(jnp.int32, (toks, experts * cap), 1).astype(jnp.float32)
    picks = [(lanes == place).astype(jnp.float32).astype(jnp.bfloat16) for place in places]
    step = 4 * LANE
    for n in range(width // step):
        cut = pl.ds(n * step, step)
        rows = ret[:, :, cut].reshape(experts * cap, step)
        total = jnp.zeros((toks, step), jnp.float32)
        for m in range(2):
            total = total + weight_ref[:, m:m + 1] * jnp.dot(
                picks[m], rows, preferred_element_type=jnp.float32)
        out_ref[:, cut] = total.astype(jnp.bfloat16)


def local(tokens, norm_gain, expert_ids, route_weights, w_gate, w_up, w_down):
    experts = lax.axis_size("ep") // 2
    toks, width = tokens.shape
    hidden = w_gate.shape[1]
    capacity = 2 * max(1, 5 * toks * expert_ids.shape[1] // (8 * experts))
    cap = -(-capacity // 16) * 16
    tiles = hidden // LANE
    vmem, any_space = pl.BlockSpec(memory_space=pltpu.VMEM), pl.BlockSpec(memory_space=pl.ANY)
    dma = pltpu.SemaphoreType.DMA
    bf16 = jnp.bfloat16
    return pl.pallas_call(
        functools.partial(kernel, experts, cap),
        out_shape=jax.ShapeDtypeStruct((toks, width), bf16),
        in_specs=[vmem] * 5 + [any_space] * 3,
        out_specs=vmem,
        scratch_shapes=[
            pltpu.VMEM((toks, width), bf16),
            pltpu.VMEM((experts, cap, width), bf16),
            pltpu.VMEM((experts * 4, cap, width), bf16),
            pltpu.VMEM((4 * cap, hidden), bf16),
            pltpu.VMEM((experts * 4, cap, width), bf16),
            pltpu.VMEM((experts * 2, cap, width), bf16),
            pltpu.VMEM((experts * 2, cap, width), bf16),
            pltpu.VMEM((experts, cap, width), bf16),
            pltpu.VMEM((experts, cap, width), bf16),
            pltpu.VMEM((experts, cap, width), bf16),
            pltpu.VMEM((tiles, width, 2 * LANE), bf16),
            pltpu.VMEM((hidden, width), bf16),
            dma((tiles,)), dma((tiles,)), dma, dma,
        ] + [dma((experts,))] * 8 + [dma((2 * experts,))] * 2 + [dma((experts,))] * 4,
        compiler_params=pltpu.CompilerParams(
            collective_id=0, has_side_effects=True, vmem_limit_bytes=60 * 1024 * 1024),
    )(tokens, norm_gain.reshape(1, -1), expert_ids, expert_ids.T, route_weights, w_gate, w_up, w_down)


def solution(mesh):
    placed = (
        P(("grp", "ep", "tp"), None),
        P(),
        P(("grp", "ep", "tp"), None),
        P(("grp", "ep", "tp"), None),
        P(None, ("ep", "tp")),
        P(None, ("ep", "tp")),
        P(("ep", "tp"), None),
    )
    return jax.shard_map(
        local, mesh=mesh, in_specs=placed, out_specs=P(("grp", "ep", "tp"), None), check_vma=False
    )
```

```python
import functools

import jax
import jax.numpy as jnp
from jax import lax
from jax.experimental import pallas as pl
from jax.experimental.pallas import tpu as pltpu
from jax.sharding import PartitionSpec as P

MESH = pl.DeviceIdType.MESH
LANE = 128
PIECES = 2


def turn(i, experts):
    return i % experts


def mix_index(first, second, count):
    total = first * 0
    bit = 1
    while bit < count:
        one, two = (first // bit) % 2, (second // bit) % 2
        total = total + bit * (one + two - 2 * one * two)
        bit *= 2
    return total


def kernel(
    experts, cap,
    tok_ref, gain_ref, ids_ref, weight_ref, gate_ref, up_ref, down_ref,
    out_ref,
    norm, xs, xa, hid, po, rd, cx, rx, fo, ret, wgu, wd,
    gate_sem, up_sem, down_sem, own_sem,
    z_send, z_recv, x_send, x_recv, d_send, d_recv, e_send, e_recv,
    r_send, r_recv, v_send, v_recv, w_send, w_recv,
):
    ep, c = lax.axis_index("ep"), lax.axis_index("tp")
    p, h = ep // 2, ep % 2
    toks, width = tok_ref.shape
    tiles = wgu.shape[0]
    part_width = width // PIECES
    across = {"ep": 2 * p + 1 - h, "tp": c}
    beside = {"ep": ep, "tp": 1 - c}

    def plane(q):
        return {"ep": 2 * q + h, "tp": c}

    barrier = pltpu.get_barrier_semaphore()

    def greet(k, carry):
        pl.semaphore_signal(barrier, inc=1, device_id=plane(mix_index(p, k, experts)), device_id_type=MESH)
        return carry

    lax.fori_loop(1, experts, greet, 0)
    pl.semaphore_signal(barrier, inc=1, device_id=across, device_id_type=MESH)
    pl.semaphore_signal(barrier, inc=1, device_id=beside, device_id_type=MESH)

    def gate_copy(j):
        return pltpu.make_async_copy(
            gate_ref.at[:, pl.ds(j * LANE, LANE)], wgu.at[j, :, pl.ds(0, LANE)], gate_sem.at[j])

    def up_copy(j):
        return pltpu.make_async_copy(
            up_ref.at[:, pl.ds(j * LANE, LANE)], wgu.at[j, :, pl.ds(LANE, LANE)], up_sem.at[j])

    down_copy = pltpu.make_async_copy(down_ref, wd, down_sem)
    for j in range(tiles):
        gate_copy(j).start()
        up_copy(j).start()
    down_copy.start()

    values = tok_ref[...].astype(jnp.float32)
    scale_rows = lax.rsqrt(jnp.mean(values * values, axis=1, keepdims=True) + 1e-06)
    norm[...] = (values * scale_rows * gain_ref[...]).astype(jnp.bfloat16)

    row = lax.broadcasted_iota(jnp.int32, (toks, toks), 0)
    col = lax.broadcasted_iota(jnp.int32, (toks, toks), 1)
    before = (row < col).astype(jnp.float32).astype(jnp.bfloat16)
    slots = lax.broadcasted_iota(jnp.int32, (cap, toks), 0).astype(jnp.float32)

    def remote(src, dst, send, recv, target):
        return pltpu.make_async_remote_copy(
            src_ref=src, dst_ref=dst, send_sem=send, recv_sem=recv, device_id=target, device_id_type=MESH)

    def cut(ref, index, g):
        return ref.at[index, :, pl.ds(g * part_width, part_width)]

    def z_pair(k, g, origin):
        q = mix_index(p, k, experts)
        n = PIECES * k + g
        return remote(
            cut(xs, q, g), cut(xa, 4 * origin(q) + 2 * h + c, g), z_send.at[n], z_recv.at[n], plane(q))

    def z_copy(k, g):
        return z_pair(k, g, lambda q: p)

    def z_land(k, g):
        return z_pair(k, g, lambda q: q)

    own_copy = pltpu.make_async_copy(xs.at[p], xa.at[4 * p + 2 * h + c], own_sem)

    def mine(k, half, core, g):
        return cut(xa, 4 * mix_index(p, k, experts) + 2 * half + core, g)

    def shift(k, g, there, here, send, recv, target):
        n = PIECES * k + g
        return remote(mine(k, *there, g), mine(k, *here, g), send.at[n], recv.at[n], target)

    def x_copy(k, g):
        return shift(k, g, (h, c), (h, c), x_send, x_recv, across)

    def x_land(k, g):
        return shift(k, g, (h, c), (1 - h, c), x_send, x_recv, across)

    def d_copy(k, g):
        return shift(k, g, (h, c), (h, c), d_send, d_recv, beside)

    def d_land(k, g):
        return shift(k, g, (h, c), (h, 1 - c), d_send, d_recv, beside)

    def e_copy(k, g):
        return shift(k, g, (1 - h, c), (1 - h, c), e_send, e_recv, beside)

    def e_land(k, g):
        return shift(k, g, (1 - h, c), (1 - h, 1 - c), e_send, e_recv, beside)

    def r_copy(k, half, g):
        n = 2 * (PIECES * k + g) + half
        return remote(
            cut(po, 4 * k + 2 * half + 1 - c, g), cut(rd, 2 * k + half, g),
            r_send.at[n], r_recv.at[n], beside)

    def v_copy(k, g):
        n = PIECES * k + g
        return remote(cut(cx, 2 * k + 1 - h, g), cut(rx, k, g), v_send.at[n], v_recv.at[n], across)

    def w_pair(k, g, origin):
        q = mix_index(p, k, experts)
        n = PIECES * k + g
        return remote(cut(fo, k, g), cut(ret, origin(q), g), w_send.at[n], w_recv.at[n], plane(q))

    def w_copy(k, g):
        return w_pair(k, g, lambda q: p)

    def w_land(k, g):
        return w_pair(k, g, lambda q: q)

    pl.semaphore_wait(barrier, experts + 1)

    def fill(i, carry):
        k = turn(i + 1, experts)
        e = mix_index(p, k, experts)
        named = ((ids_ref[0:1, :] == e) | (ids_ref[1:2, :] == e)).astype(jnp.float32)
        rank = jnp.dot(
            jnp.broadcast_to(named, (16, toks)).astype(jnp.bfloat16), before,
            preferred_element_type=jnp.float32)[0:1, :]
        pick = jnp.where(slots == rank, named, 0.0).astype(jnp.bfloat16)
        xs[e] = jnp.dot(pick, norm[...], preferred_element_type=jnp.float32).astype(jnp.bfloat16)

        @pl.when(k > 0)
        def _():
            for g in range(PIECES):
                z_copy(k, g).start()

        return carry

    lax.fori_loop(0, experts, fill, 0)
    own_copy.start()
    own_copy.wait()

    step = 2 * LANE

    def compute(k):
        first = 4 * mix_index(p, k, experts)

        def gate_up(j, carry):
            rows = xa[pl.ds(first, 4)].reshape(4 * cap, width)
            both = jnp.dot(rows, wgu[j], preferred_element_type=jnp.float32)
            gate, up = both[:, :LANE], both[:, LANE:]
            hid[:, pl.ds(pl.multiple_of(j * LANE, LANE), LANE)] = (
                gate / (1.0 + jnp.exp(-gate)) * up).astype(jnp.bfloat16)
            return carry

        lax.fori_loop(0, tiles, gate_up, 0)

        def down(n, carry):
            place = pl.ds(pl.multiple_of(n * step, step), step)
            part = jnp.dot(hid[...], wd[:, place], preferred_element_type=jnp.float32)
            po[pl.ds(4 * k, 4), :, place] = part.astype(jnp.bfloat16).reshape(4, cap, step)
            return carry

        many = part_width // step
        for g in range(PIECES):
            lax.fori_loop(g * many, (g + 1) * many, down, 0)
            for half in range(2):
                r_copy(k, half, g).start()

    def add(first, second):
        return (first.astype(jnp.float32) + second.astype(jnp.float32)).astype(jnp.bfloat16)

    def finish(k):
        for g in range(PIECES):
            v_copy(k, g).wait_recv()
            cols = pl.ds(g * part_width, part_width)
            total = add(cx[2 * k + h, :, cols], rx[k, :, cols])

            @pl.when(k == 0)
            def _():
                ret[p, :, cols] = total

            @pl.when(k > 0)
            def _():
                fo[k, :, cols] = total
                w_copy(k, g).start()

    def stage(i, carry):
        @pl.when(i < experts)
        def _():
            k = turn(i, experts)
            for g in range(PIECES):
                @pl.when(k > 0)
                def _():
                    z_land(k, g).wait_recv()

                x_copy(k, g).start()
                d_copy(k, g).start()

        @pl.when(i > 0)
        def _():
            k = turn(i - 1, experts)
            for g in range(PIECES):
                x_land(k, g).wait_recv()
                e_copy(k, g).start()

            @pl.when(i == 1)
            def _():
                for j in range(tiles):
                    gate_copy(j).wait()
                    up_copy(j).wait()
                down_copy.wait()

            for g in range(PIECES):
                d_land(k, g).wait_recv()
                e_land(k, g).wait_recv()
            compute(k)

            @pl.when(i > 2)
            def _():
                finish(turn(i - 2, experts))

            for g in range(PIECES):
                cols = pl.ds(g * part_width, part_width)
                for half in range(2):
                    r_copy(k, half, g).wait_recv()
                    cx[2 * k + half, :, cols] = add(
                        po[4 * k + 2 * half + c, :, cols], rd[2 * k + half, :, cols])

                @pl.when(k > 0)
                def _():
                    v_copy(k, g).start()

        return carry

    lax.fori_loop(0, experts + 1, stage, 0)
    for g in range(PIECES):
        v_copy(0, g).start()

    def settle(k, carry):
        for g in range(PIECES):
            x_copy(k, g).wait_send()
            d_copy(k, g).wait_send()
            e_copy(k, g).wait_send()
            r_copy(k, 0, g).wait_send()
            r_copy(k, 1, g).wait_send()
            v_copy(k, g).wait_send()

            @pl.when(k > 0)
            def _():
                z_copy(k, g).wait_send()
                w_copy(k, g).wait_send()

        return carry

    after = (col < row).astype(jnp.float32).astype(jnp.bfloat16)

    sides = jnp.concatenate(
        [ids_ref[...].astype(jnp.float32), weight_ref[...], jnp.zeros((LANE - 4, toks), jnp.float32)], axis=0).T

    def place_of(e, places):
        number = lax.convert_element_type(e, jnp.float32)
        hits = [(sides[:, n:n + 1] == number).astype(jnp.float32) for n in range(2)]
        rank = jnp.dot(
            after, jnp.broadcast_to(hits[0] + hits[1], (toks, LANE)).astype(jnp.bfloat16),
            preferred_element_type=jnp.float32)[:, 0:1]
        spot = rank + number * cap
        return tuple(old + hit * spot for old, hit in zip(places, hits))

    zero = jnp.zeros((toks, 1), jnp.float32)
    places = lax.fori_loop(0, experts, place_of, (zero, zero))
    lanes = lax.broadcasted_iota(jnp.int32, (toks, experts * cap), 1).astype(jnp.float32)
    picks = [(lanes == place).astype(jnp.float32).astype(jnp.bfloat16) for place in places]
    finish(turn(experts - 1, experts))
    finish(0)
    lax.fori_loop(0, experts, settle, 0)
    for g in range(PIECES):
        def landed(k, carry):
            w_land(k, g).wait_recv()
            return carry

        lax.fori_loop(1, experts, landed, 0)
        cols = pl.ds(g * part_width, part_width)
        rows = ret[:, :, cols].reshape(experts * cap, part_width)
        total = jnp.zeros((toks, part_width), jnp.float32)
        for m in range(2):
            total = total + sides[:, 2 + m:3 + m] * jnp.dot(
                picks[m], rows, preferred_element_type=jnp.float32)
        out_ref[:, cols] = total.astype(jnp.bfloat16)


def local(tokens, norm_gain, expert_ids, route_weights, w_gate, w_up, w_down):
    experts = lax.axis_size("ep") // 2
    toks, width = tokens.shape
    hidden = w_gate.shape[1]
    capacity = 2 * max(1, 5 * toks * expert_ids.shape[1] // (8 * experts))
    cap = -(-capacity // 16) * 16
    tiles = hidden // LANE
    vmem, any_space = pl.BlockSpec(memory_space=pltpu.VMEM), pl.BlockSpec(memory_space=pl.ANY)
    dma = pltpu.SemaphoreType.DMA
    bf16 = jnp.bfloat16
    return pl.pallas_call(
        functools.partial(kernel, experts, cap),
        out_shape=jax.ShapeDtypeStruct((toks, width), bf16),
        in_specs=[vmem] * 4 + [any_space] * 3,
        out_specs=vmem,
        scratch_shapes=[
            pltpu.VMEM((toks, width), bf16),
            pltpu.VMEM((experts, cap, width), bf16),
            pltpu.VMEM((experts * 4, cap, width), bf16),
            pltpu.VMEM((4 * cap, hidden), bf16),
            pltpu.VMEM((experts * 4, cap, width), bf16),
            pltpu.VMEM((experts * 2, cap, width), bf16),
            pltpu.VMEM((experts * 2, cap, width), bf16),
            pltpu.VMEM((experts, cap, width), bf16),
            pltpu.VMEM((experts, cap, width), bf16),
            pltpu.VMEM((experts, cap, width), bf16),
            pltpu.VMEM((tiles, width, 2 * LANE), bf16),
            pltpu.VMEM((hidden, width), bf16),
            dma((tiles,)), dma((tiles,)), dma, dma,
        ] + [dma((PIECES * experts,))] * 8 + [dma((2 * PIECES * experts,))] * 2 + [dma((PIECES * experts,))] * 4,
        compiler_params=pltpu.CompilerParams(
            collective_id=0, has_side_effects=True, vmem_limit_bytes=60 * 1024 * 1024),
    )(tokens, norm_gain.reshape(1, -1), expert_ids.T, route_weights.T, w_gate, w_up, w_down)


def solution(mesh):
    placed = (
        P(("grp", "ep", "tp"), None),
        P(),
        P(("grp", "ep", "tp"), None),
        P(("grp", "ep", "tp"), None),
        P(None, ("ep", "tp")),
        P(None, ("ep", "tp")),
        P(("ep", "tp"), None),
    )
    return jax.shard_map(
        local, mesh=mesh, in_specs=placed, out_specs=P(("grp", "ep", "tp"), None), check_vma=False
    )
```
